32 devices in a mesh: fs: 8 (over z, y), tp: 4 (over x, core).
Axes of the slice: x: 2, y: 2, z: 4, core: 2. Of those that a mesh axis runs over, the one named last changes fastest.
Arguments:
- inputs: bfloat16 [6144, 2048], P('fs'), may hold values from -6 to 6
- values_cot: bfloat16 [6144, 2048], P('fs', 'tp'), may hold values from -0.22949219 to 0.22949219
- decay_cot: bfloat16 [6144, 16], P('fs'), may hold values from -0.22949219 to 0.22949219
- factor: bfloat16 [2048, 512], P('fs', 'tp'), may hold values from -0.125 to 0.125
- value_weight: float32 [2048, 2048], P('fs', 'tp'), may hold values from -3 to 3
- lowrank_mean: float32 [512, 2048], P('fs', 'tp'), may hold values from -60 to 60
- lowrank_var: float32 [512, 2048], P('fs', 'tp'), may hold values from 0.3 to 3
- decay_weight: float32 [2048, 16], replicated, may hold values from -3 to 3
- decay_mean: float32 [2048, 16], replicated, may hold values from -6 to 6
- decay_var: float32 [2048, 16], replicated, may hold values from 0.3 to 3
Outputs:
- value_step: float32 [2048, 2048], P('fs', 'tp')
- value_new: float32 [2048, 2048], P('fs', 'tp')
- value_copy: bfloat16 [2048, 2048], P('fs', 'tp')
- mean_new: float32 [512, 2048], P('fs', 'tp')
- var_new: float32 [512, 2048], P('fs', 'tp')
- decay_new: float32 [2048, 16], replicated
- decay_copy: bfloat16 [2048, 16], replicated
- decay_mean_new: float32 [2048, 16], replicated
- decay_var_new: float32 [2048, 16], replicated
The draws below stay inside these ranges and needn't reach their ends.
All inputs are finite; a program needn't handle non-finite values.
Results may differ from the reference program's by a relative error of at most 0.0042.
Values may be sent and summed in bfloat16 or wider, within the bound.
A program may use at most 64 MiB of HBM per device.

```python
import math
import jax
import jax.numpy as jnp
from jax import lax

D = 2048
W = 2048
H = 16
R = 512
TOKENS = 6144


def draw_lowrank_mean(key, part):
    base = jnp.clip(jax.random.normal(key, (R, W), jnp.float32), -6.0, 6.0)
    row_scale = 10.0 ** (0.5 * jnp.arange(R, dtype=jnp.float32) / R)
    col_scale = 10.0 ** (0.5 * jnp.arange(W, dtype=jnp.float32) / W)
    return base * row_scale[:, None] * col_scale[None, :]


def steps_of(key, shape, cuts, least, largest):
    level = 1.0
    for axis_at, parts in cuts:
        draws = jax.random.uniform(jax.random.fold_in(jax.random.fold_in(key, 6), axis_at), (parts,), jnp.float32, least / len(cuts), largest / len(cuts))
        level = level * jnp.repeat(jnp.exp(draws), shape[axis_at] // parts).reshape((-1,) + (1,) * (len(shape) - 1 - axis_at))
    return level


def noise(rng, shape, deviation, bound, pieces=(), held_as=jnp.bfloat16):
    entries = deviation * jax.random.normal(rng, shape, jnp.float32)
    if pieces:
        entries = entries * steps_of(rng, shape, pieces, -0.22, 0.18)
    return jnp.clip(entries, -bound, bound).astype(held_as)


def setup_inputs(seed: int = 0) -> dict:
    key_of = jax.random.split(jax.random.key(seed), 11)
    inputs = noise(key_of[0], (TOKENS, D), 1.0, 6.0, ((0, 8),))
    values_cot = noise(key_of[1], (TOKENS, W), (3.0 * TOKENS ** -0.5), 0.22949219, ((0, 8), (1, 4)))
    decay_cot = noise(key_of[2], (TOKENS, H), (3.0 * TOKENS ** -0.5), 0.22949219, ((0, 8),))
    factor = noise(key_of[3], (D, R), D ** -0.5, 0.125, ((0, 8), (1, 4)))
    value_weight = noise(key_of[4], (D, W), 0.5, 3.0, ((0, 8), (1, 4)), jnp.float32)
    lowrank_mean = draw_lowrank_mean(jax.random.fold_in(key_of[10], 71), 0)
    lowrank_var = jnp.clip(jnp.exp(math.log(3.0) - 2.3025851 * jax.random.uniform(key_of[6], (R, W), jnp.float32) ** steps_of(key_of[6], (R, W), ((0, 8), (1, 4)), -0.2, 0.2)), 0.3, 3.0)
    decay_weight = noise(key_of[7], (D, H), 0.5, 3.0, (), jnp.float32)
    decay_mean = noise(key_of[8], (D, H), 1.0, 6.0, (), jnp.float32)
    decay_var = jnp.clip(jnp.exp(jax.random.uniform(key_of[9], (D, H), jnp.float32, math.log(0.3), math.log(3.0))), 0.3, 3.0)
    return {"inputs": inputs, "values_cot": values_cot, "decay_cot": decay_cot, "factor": factor, "value_weight": value_weight, "lowrank_mean": lowrank_mean, "lowrank_var": lowrank_var, "decay_weight": decay_weight, "decay_mean": decay_mean, "decay_var": decay_var}


def reference(inputs, values_cot, decay_cot, factor, value_weight, lowrank_mean, lowrank_var, decay_weight, decay_mean, decay_var):
    projected = jnp.dot(inputs, factor, preferred_element_type=jnp.float32).astype(jnp.bfloat16)
    lowrank_grad = lax.dot_general(projected, values_cot, (((0,), (0,)), ((), ())), preferred_element_type=jnp.float32)
    mean_new = 0.9 * lowrank_mean + 0.1 * lowrank_grad
    var_new = 0.95 * lowrank_var + 0.05 * lowrank_grad * lowrank_grad
    adam_ratio = mean_new / (jnp.sqrt(var_new) + 1e-08)
    root_mean = jnp.sqrt(jnp.sum(adam_ratio * adam_ratio) / (R * W) + 1e-06)
    delta = jnp.dot(factor.astype(jnp.float32), adam_ratio, precision=lax.Precision.HIGHEST)
    value_step = -0.5 / root_mean * delta
    value_new = value_weight + value_step
    value_copy = value_new.astype(jnp.bfloat16)
    decay_grad = lax.dot_general(inputs, decay_cot, (((0,), (0,)), ((), ())), preferred_element_type=jnp.float32)
    decay_mean_new = 0.9 * decay_mean + 0.1 * decay_grad
    decay_var_new = 0.95 * decay_var + 0.05 * decay_grad * decay_grad
    decay_new = decay_weight - 0.5 * decay_mean_new / (jnp.sqrt(decay_var_new) + 1e-08)
    decay_copy = decay_new.astype(jnp.bfloat16)
    return (value_step, value_new, value_copy, mean_new, var_new, decay_new, decay_copy, decay_mean_new, decay_var_new)
```

```python
import functools

import jax
import jax.numpy as jnp
from jax import lax
from jax.experimental import pallas as pl
from jax.experimental.pallas import tpu as pltpu
from jax.sharding import PartitionSpec as P

MESH = pl.DeviceIdType.MESH
F32 = jnp.float32
BF16 = jnp.bfloat16


def moments(mean, var, grad):
    return 0.9 * mean + 0.1 * grad, 0.95 * var + 0.05 * grad * grad


def remote(src, dst, send_sem, recv_sem, axis, peer):
    return pltpu.make_async_remote_copy(
        src_ref=src,
        dst_ref=dst,
        send_sem=send_sem,
        recv_sem=recv_sem,
        device_id={axis: peer},
        device_id_type=MESH,
    )


class Gather:
    def __init__(self, axis, size, view, send_sems, recv_sems, pending):
        self.axis, self.view, self.pending = axis, view, pending
        self.send_sems, self.recv_sems = send_sems, recv_sems
        self.me = lax.axis_index(axis)
        self.groups = size // 2
        self.group, self.parity = self.me // 2, self.me % 2
        self.partner = self.group * 2 + 1 - self.parity
        self.steps = sorted(range(1, self.groups), key=lambda d: min(d, self.groups - d))

    def slot(self, step, parity):
        return (self.group + step) % self.groups * 2 + parity

    def send(self, block, peer, number):
        ref = self.view(block)
        copy = remote(ref, ref, self.send_sems.at[number], self.recv_sems.at[block], self.axis, peer)
        copy.start()
        self.pending.append(copy)

    def wait(self, block):
        ref = self.view(block)
        remote(ref, ref, self.send_sems.at[0], self.recv_sems.at[block], self.axis, self.partner).wait_recv()

    def start(self):
        for number, step in enumerate(self.steps):
            self.send(self.me, self.slot(step, self.parity), number)
        self.send(self.me, self.partner, self.groups - 1)

    def arrivals(self):
        self.wait(self.partner)
        yield self.partner
        for number, step in enumerate(self.steps):
            block = self.slot(step, self.parity)
            self.wait(block)
            self.send(block, self.partner, self.groups + number)
            yield block
        for step in self.steps:
            block = self.slot(step, 1 - self.parity)
            self.wait(block)
            yield block


class Spread:
    def __init__(self, axis, size, view, send_sems, recv_sems, pending):
        self.axis, self.size, self.view, self.pending = axis, size, view, pending
        self.send_sems, self.recv_sems = send_sems, recv_sems
        self.me = lax.axis_index(axis)

    def start(self):
        ref = self.view(self.me)
        for step in range(1, self.size):
            copy = remote(
                ref, ref, self.send_sems.at[step - 1], self.recv_sems.at[self.me], self.axis, (self.me + step) % self.size
            )
            copy.start()
            self.pending.append(copy)

    def finish(self):
        for step in range(1, self.size):
            source = (self.me + step) % self.size
            ref = self.view(source)
            remote(ref, ref, self.send_sems.at[0], self.recv_sems.at[source], self.axis, source).wait_recv()


def rows_of(ref, size):
    return lambda i: ref.at[pl.ds(pl.multiple_of(i * size, size), size)]


def columns_of(ref, size):
    return lambda i: ref.at[:, pl.ds(pl.multiple_of(i * size, size), size)]


def kernel(
    n,
    t,
    inputs_hbm,
    values_hbm,
    decay_hbm,
    factor_hbm,
    mean_hbm,
    var_hbm,
    delta_ref,
    square_ref,
    grad_ref,
    decay_grad_ref,
    inputs,
    values,
    decay,
    mean,
    var,
    quarter,
    own_rows,
    total,
    projected,
    partial,
    out_y,
    in_y,
    out_z,
    in_z,
    ratio,
    decay_parts,
    square_tp,
    square_fs,
    load_sems,
    a_send,
    a_recv,
    o_send,
    o_recv,
    b_send,
    b_recv,
    y_send,
    y_recv,
    z_send,
    z_recv,
    d_send,
    d_recv,
    p_send,
    p_recv,
    q_send,
    q_recv,
    st_send,
    st_recv,
    sf_send,
    sf_recv,
):
    fs, tp = lax.axis_index("fs"), lax.axis_index("tp")
    group, parity = fs // 2, fs % 2
    partner = group * 2 + 1 - parity
    depth, width = factor_hbm.shape
    rank = width * t
    block_rows, owner_rows = rank // t, rank // n
    decay_width = inputs.shape[1] // t
    pending = []

    quarter_view = rows_of(quarter, depth)
    own_view = columns_of(own_rows, width)
    loads = [
        pltpu.make_async_copy(source, target, load_sems.at[i])
        for i, (source, target) in enumerate(
            (
                (factor_hbm, quarter_view(fs)),
                (factor_hbm, own_view(tp)),
                (decay_hbm, decay),
                (inputs_hbm, inputs),
                (values_hbm, values),
                (mean_hbm, mean),
                (var_hbm, var),
            )
        )
    ]
    for load in loads:
        load.start()

    barrier = pltpu.get_barrier_semaphore()
    for step in range(1, t):
        pl.semaphore_signal(barrier, inc=1, device_id={"tp": (tp + step) % t}, device_id_type=MESH)
    for step in range(1, n):
        pl.semaphore_signal(barrier, inc=1, device_id={"fs": (fs + step) % n}, device_id_type=MESH)
    pl.semaphore_wait(barrier, n + t - 2)

    a = Gather("fs", n, quarter_view, a_send, a_recv, pending)
    loads[0].wait()
    a.start()
    own = Gather("tp", t, own_view, o_send, o_recv, pending)
    loads[1].wait()
    own.start()

    loads[2].wait()
    loads[3].wait()
    decay_columns = pl.ds(pl.multiple_of(tp * decay_width, decay_width), decay_width)
    decay_parts[fs] = jnp.dot(decay[...], inputs[:, decay_columns], preferred_element_type=F32).astype(BF16)

    def project(block):
        at = pl.ds(pl.multiple_of(block * depth, depth), depth)
        return jnp.dot(inputs[:, at], quarter[at], preferred_element_type=F32)

    total[...] = project(fs)
    for block in a.arrivals():
        total[...] += project(block)

    projected_view = rows_of(projected, block_rows)
    projected_view(tp)[...] = total[...].T.astype(BF16)
    b = Gather("tp", t, projected_view, b_send, b_recv, pending)
    b.start()
    p = Spread("fs", n, lambda i: decay_parts.at[i], p_send, p_recv, pending)
    p.start()

    out_y_view, in_y_view = rows_of(out_y, owner_rows), rows_of(in_y, owner_rows)
    out_z_view, in_z_view = rows_of(out_z, owner_rows), rows_of(in_z, owner_rows)
    partial_view = rows_of(partial, owner_rows)
    per = n // t // 2

    def reduce_pair(block):
        rows_of(partial, block_rows)(block)[...] = jnp.dot(
            projected_view(block)[...], values[...], preferred_element_type=F32
        )
        for j in range(per):
            target = block * per + j
            out_y_view(target)[...] = partial_view(target * 2 + 1 - parity)[...].astype(BF16)
            copy = remote(
                out_y_view(target), in_y_view(target), y_send.at[target], y_recv.at[target], "fs", partner
            )
            copy.start()
            pending.append(copy)

    def reduce_groups(block):
        for j in range(per):
            target = block * per + j
            remote(
                out_y_view(target), in_y_view(target), y_send.at[target], y_recv.at[target], "fs", partner
            ).wait_recv()
            mine = partial_view(target * 2 + parity)
            mine[...] = mine[...] + in_y_view(target)[...].astype(F32)
            out_z_view(target)[...] = mine[...].astype(BF16)

            @pl.when(target != group)
            def _():
                remote(
                    out_z_view(target),
                    in_z_view(group),
                    z_send.at[target],
                    z_recv.at[group],
                    "fs",
                    target * 2 + parity,
                ).start()

    loads[4].wait()
    reduce_pair(tp)
    waiting = [tp]
    blocks = b.arrivals()
    for number in range(1, t):
        block = next(blocks)
        reduce_pair(block)
        waiting.append(block)
        if number % 2 == 1:
            for each in waiting:
                reduce_groups(each)
            waiting = []
    for _ in blocks:
        pass

    p.finish()
    decay_sum = decay_parts[0].astype(F32)
    for i in range(1, n):
        decay_sum += decay_parts[i].astype(F32)
    decay_grad_ref[:, decay_columns] = decay_sum
    q = Spread("tp", t, columns_of(decay_grad_ref, decay_width), q_send, q_recv, pending)
    q.start()
    for _ in own.arrivals():
        pass

    loads[5].wait()
    loads[6].wait()
    grad = partial_view(fs)[...]
    for step in range(1, n // 2):
        source = (group + step) % (n // 2)
        remote(
            out_z_view(source), in_z_view(source), z_send.at[source], z_recv.at[source], "fs", source * 2 + parity
        ).wait_recv()
        grad += in_z_view(source)[...].astype(F32)
    grad_ref[...] = grad
    mean_new, var_new = moments(mean[...], var[...], grad)
    adam_ratio = mean_new / (jnp.sqrt(var_new) + 1e-08)
    ratio_view = rows_of(ratio, owner_rows)
    ratio_view(fs)[...] = adam_ratio.astype(BF16)
    d = Gather("fs", n, ratio_view, d_send, d_recv, pending)
    d.start()

    squares = adam_ratio * adam_ratio
    squares = sum(squares[i : i + 8] for i in range(0, squares.shape[0], 8))
    square_tp[tp] = sum(squares[:, i : i + 128] for i in range(0, squares.shape[1], 128))
    st = Spread("tp", t, lambda i: square_tp.at[i], st_send, st_recv, pending)
    st.start()
    st.finish()
    square_fs[fs] = sum(square_tp[i] for i in range(t))
    sf = Spread("fs", n, lambda i: square_fs.at[i], sf_send, sf_recv, pending)
    sf.start()

    for _ in d.arrivals():
        pass
    delta_ref[...] = jnp.dot(own_rows[...], ratio[...], preferred_element_type=F32)
    sf.finish()
    square_ref[...] = sum(square_fs[i] for i in range(n))
    q.finish()
    for copy in pending:
        copy.wait_send()
    for step in range(1, n // 2):
        target = (group + step) % (n // 2)
        remote(
            out_z_view(target), in_z_view(target), z_send.at[target], z_recv.at[target], "fs", target * 2 + parity
        ).wait_send()


def fits(n, t, inputs, decay_cot, factor, mean):
    depth, width = factor.shape
    rank = width * t
    return (
        n % (2 * t) == 0
        and t % 2 == 0
        and mean.shape[0] % 16 == 0
        and mean.shape[1] % 128 == 0
        and mean.shape[0] * n == rank
        and depth % 128 == 0
        and width % 128 == 0
        and inputs.shape[0] % 128 == 0
        and inputs.shape[1] % (128 * t) == 0
        and decay_cot.shape[1] % 16 == 0
    )


def by_kernel(n, t, inputs, values_cot, decay_cot, factor, mean, var):
    tokens, model = inputs.shape
    depth, width = factor.shape
    columns = values_cot.shape[1]
    heads = decay_cot.shape[1]
    rank = width * t
    owner_rows = rank // n
    dma = lambda k: pltpu.SemaphoreType.DMA((k,))
    half = n // 2
    delta, square, grad, decay_grad = pl.pallas_call(
        functools.partial(kernel, n, t),
        out_shape=(
            jax.ShapeDtypeStruct((depth, columns), F32),
            jax.ShapeDtypeStruct((8, 128), F32),
            jax.ShapeDtypeStruct((owner_rows, columns), F32),
            jax.ShapeDtypeStruct((heads, model), F32),
        ),
        in_specs=[pl.BlockSpec(memory_space=pl.ANY)] * 6,
        out_specs=[pl.BlockSpec(memory_space=pltpu.VMEM)] * 4,
        scratch_shapes=[
            pltpu.VMEM((tokens, model), BF16),
            pltpu.VMEM((tokens, columns), BF16),
            pltpu.VMEM((heads, tokens), BF16),
            pltpu.VMEM((owner_rows, columns), F32),
            pltpu.VMEM((owner_rows, columns), F32),
            pltpu.VMEM((model, width), BF16),
            pltpu.VMEM((depth, rank), BF16),
            pltpu.VMEM((tokens, width), F32),
            pltpu.VMEM((rank, tokens), BF16),
            pltpu.VMEM((rank, columns), F32),
            pltpu.VMEM((rank // 2, columns), BF16),
            pltpu.VMEM((rank // 2, columns), BF16),
            pltpu.VMEM((rank // 2, columns), BF16),
            pltpu.VMEM((rank // 2, columns), BF16),
            pltpu.VMEM((rank, columns), BF16),
            pltpu.VMEM((n, heads, model // t), BF16),
            pltpu.VMEM((t, 8, 128), F32),
            pltpu.VMEM((n, 8, 128), F32),
            dma(7),
            dma(n),
            dma(n),
            dma(t),
            dma(t),
            dma(t),
            dma(t),
            dma(half),
            dma(half),
            dma(half),
            dma(half),
            dma(n),
            dma(n),
            dma(n),
            dma(n),
            dma(t),
            dma(t),
            dma(t),
            dma(t),
            dma(n),
            dma(n),
        ],
        compiler_params=pltpu.CompilerParams(collective_id=0, has_side_effects=True),
        name="lowrank",
    )(inputs, values_cot, decay_cot.T, factor, mean, var)
    return delta, jnp.sum(square), grad, decay_grad.T


def by_collectives(inputs, values_cot, decay_cot, factor, mean, var):
    own_rows = lax.all_gather(factor, "tp", axis=1, tiled=True)
    quarter = jnp.dot(
        inputs, lax.all_gather(factor, "fs", axis=0, tiled=True), preferred_element_type=F32
    ).astype(BF16)
    projected = lax.all_gather(quarter, "tp", axis=1, tiled=True)
    grad = lax.psum_scatter(
        lax.dot_general(projected, values_cot, (((0,), (0,)), ((), ())), preferred_element_type=F32),
        "fs",
        scatter_dimension=0,
        tiled=True,
    )
    mean_new, var_new = moments(mean, var, grad)
    adam_ratio = mean_new / (jnp.sqrt(var_new) + 1e-08)
    full_ratio = lax.all_gather(adam_ratio, "fs", axis=0, tiled=True)
    squares = lax.psum(jnp.sum(adam_ratio * adam_ratio), ("fs", "tp"))
    delta = jnp.dot(own_rows.astype(F32), full_ratio, precision=lax.Precision.HIGHEST)
    decay_part = lax.dot_general(inputs, decay_cot, (((0,), (0,)), ((), ())), preferred_element_type=F32)
    return delta, squares, grad, lax.psum(decay_part, "fs")


def local(
    n,
    t,
    inputs,
    values_cot,
    decay_cot,
    factor,
    value_weight,
    lowrank_mean,
    lowrank_var,
    decay_weight,
    decay_mean,
    decay_var,
):
    middle = inputs, values_cot, decay_cot, factor, lowrank_mean, lowrank_var
    if fits(n, t, inputs, decay_cot, factor, lowrank_mean):
        delta, squares, lowrank_grad, decay_grad = by_kernel(n, t, *middle)
    else:
        delta, squares, lowrank_grad, decay_grad = by_collectives(*middle)
    entries = lowrank_mean.size * n * t
    mean_new, var_new = moments(lowrank_mean, lowrank_var, lowrank_grad)
    root_mean = jnp.sqrt(squares / entries + 1e-06)
    value_step = -0.5 / root_mean * delta
    value_new = value_weight + value_step
    value_copy = value_new.astype(BF16)
    decay_mean_new, decay_var_new = moments(decay_mean, decay_var, decay_grad)
    decay_new = decay_weight - 0.5 * decay_mean_new / (jnp.sqrt(decay_var_new) + 1e-08)
    decay_copy = decay_new.astype(BF16)
    return (
        value_step,
        value_new,
        value_copy,
        mean_new,
        var_new,
        decay_new,
        decay_copy,
        decay_mean_new,
        decay_var_new,
    )


def solution(mesh):
    in_specs = (
        P("fs", None),
        P("fs", "tp"),
        P("fs", None),
        P("fs", "tp"),
        P("fs", "tp"),
        P("fs", "tp"),
        P("fs", "tp"),
        P(),
        P(),
        P(),
    )
    out_specs = (
        P("fs", "tp"),
        P("fs", "tp"),
        P("fs", "tp"),
        P("fs", "tp"),
        P("fs", "tp"),
        P(),
        P(),
        P(),
        P(),
    )
    body = functools.partial(local, mesh.shape["fs"], mesh.shape["tp"])
    return jax.shard_map(body, mesh=mesh, in_specs=in_specs, out_specs=out_specs, check_vma=False)
```

```python
import functools

import jax
import jax.numpy as jnp
from jax import lax
from jax.experimental import pallas as pl
from jax.experimental.pallas import tpu as pltpu
from jax.sharding import PartitionSpec as P

MESH = pl.DeviceIdType.MESH
F32 = jnp.float32
BF16 = jnp.bfloat16


def moments(mean, var, grad):
    return 0.9 * mean + 0.1 * grad, 0.95 * var + 0.05 * grad * grad


def remote(src, dst, send_sem, recv_sem, axis, peer):
    return pltpu.make_async_remote_copy(
        src_ref=src,
        dst_ref=dst,
        send_sem=send_sem,
        recv_sem=recv_sem,
        device_id={axis: peer},
        device_id_type=MESH,
    )


class Gather:
    def __init__(self, axis, size, view, send_sems, recv_sems, pending):
        self.axis, self.view, self.pending = axis, view, pending
        self.send_sems, self.recv_sems = send_sems, recv_sems
        self.me = lax.axis_index(axis)
        self.groups = size // 2
        self.group, self.parity = self.me // 2, self.me % 2
        self.partner = self.group * 2 + 1 - self.parity
        self.steps = sorted(range(1, self.groups), key=lambda d: min(d, self.groups - d))

    def slot(self, step, parity):
        return (self.group + step) % self.groups * 2 + parity

    def send(self, block, peer, number):
        ref = self.view(block)
        copy = remote(ref, ref, self.send_sems.at[number], self.recv_sems.at[block], self.axis, peer)
        copy.start()
        self.pending.append(copy)

    def wait(self, block):
        ref = self.view(block)
        remote(ref, ref, self.send_sems.at[0], self.recv_sems.at[block], self.axis, self.partner).wait_recv()

    def start(self):
        for number, step in enumerate(self.steps):
            self.send(self.me, self.slot(step, self.parity), number)
        self.send(self.me, self.partner, self.groups - 1)

    def arrivals(self):
        self.wait(self.partner)
        yield self.partner
        for number, step in enumerate(self.steps):
            block = self.slot(step, self.parity)
            self.wait(block)
            self.send(block, self.partner, self.groups + number)
            yield block
        for step in self.steps:
            block = self.slot(step, 1 - self.parity)
            self.wait(block)
            yield block


class Spread:
    def __init__(self, axis, size, view, send_sems, recv_sems, pending):
        self.axis, self.size, self.view, self.pending = axis, size, view, pending
        self.send_sems, self.recv_sems = send_sems, recv_sems
        self.me = lax.axis_index(axis)

    def start(self):
        ref = self.view(self.me)
        for step in range(1, self.size):
            copy = remote(
                ref, ref, self.send_sems.at[step - 1], self.recv_sems.at[self.me], self.axis, (self.me + step) % self.size
            )
            copy.start()
            self.pending.append(copy)

    def finish(self):
        for step in range(1, self.size):
            source = (self.me + step) % self.size
            ref = self.view(source)
            remote(ref, ref, self.send_sems.at[0], self.recv_sems.at[source], self.axis, source).wait_recv()


def rows_of(ref, size):
    return lambda i: ref.at[pl.ds(pl.multiple_of(i * size, size), size)]


def columns_of(ref, size):
    return lambda i: ref.at[:, pl.ds(pl.multiple_of(i * size, size), size)]


def kernel(
    n,
    t,
    inputs_hbm,
    values_hbm,
    decay_hbm,
    factor_hbm,
    mean_hbm,
    var_hbm,
    delta_ref,
    square_ref,
    grad_ref,
    decay_grad_ref,
    inputs,
    values,
    decay,
    mean,
    var,
    quarter,
    own_rows,
    total,
    projected,
    partial,
    out_y,
    in_y,
    out_z,
    in_z,
    ratio,
    decay_parts,
    square_tp,
    square_fs,
    load_sems,
    a_send,
    a_recv,
    o_send,
    o_recv,
    b_send,
    b_recv,
    y_send,
    y_recv,
    z_send,
    z_recv,
    d_send,
    d_recv,
    p_send,
    p_recv,
    q_send,
    q_recv,
    st_send,
    st_recv,
    sf_send,
    sf_recv,
):
    fs, tp = lax.axis_index("fs"), lax.axis_index("tp")
    group, parity = fs // 2, fs % 2
    partner = group * 2 + 1 - parity
    depth, width = factor_hbm.shape
    rank = width * t
    block_rows, owner_rows = rank // t, rank // n
    decay_width = inputs.shape[1] // t
    pending = []

    quarter_view = rows_of(quarter, depth)
    own_view = columns_of(own_rows, width)
    loads = [
        pltpu.make_async_copy(source, target, load_sems.at[i])
        for i, (source, target) in enumerate(
            (
                (factor_hbm, quarter_view(fs)),
                (factor_hbm, own_view(tp)),
                (decay_hbm, decay),
                (inputs_hbm, inputs),
                (values_hbm, values),
                (mean_hbm, mean),
                (var_hbm, var),
            )
        )
    ]
    for load in loads:
        load.start()

    barrier = pltpu.get_barrier_semaphore()
    for step in range(1, t):
        pl.semaphore_signal(barrier, inc=1, device_id={"tp": (tp + step) % t}, device_id_type=MESH)
    for step in range(1, n):
        pl.semaphore_signal(barrier, inc=1, device_id={"fs": (fs + step) % n}, device_id_type=MESH)
    pl.semaphore_wait(barrier, n + t - 2)

    a = Gather("fs", n, quarter_view, a_send, a_recv, pending)
    loads[0].wait()
    a.start()
    own = Gather("tp", t, own_view, o_send, o_recv, pending)
    loads[1].wait()
    own.start()

    loads[2].wait()
    loads[3].wait()
    decay_columns = pl.ds(pl.multiple_of(tp * decay_width, decay_width), decay_width)
    decay_parts[fs] = jnp.dot(decay[...], inputs[:, decay_columns], preferred_element_type=F32).astype(BF16)

    def project(block):
        at = pl.ds(pl.multiple_of(block * depth, depth), depth)
        return jnp.dot(inputs[:, at], quarter[at], preferred_element_type=F32)

    total[...] = project(fs)
    for block in a.arrivals():
        total[...] += project(block)

    projected_view = rows_of(projected, block_rows)
    projected_view(tp)[...] = total[...].T.astype(BF16)
    b = Gather("tp", t, projected_view, b_send, b_recv, pending)
    b.start()
    p = Spread("fs", n, lambda i: decay_parts.at[i], p_send, p_recv, pending)
    p.start()

    out_y_view, in_y_view = rows_of(out_y, owner_rows), rows_of(in_y, owner_rows)
    out_z_view, in_z_view = rows_of(out_z, owner_rows), rows_of(in_z, owner_rows)
    partial_view = rows_of(partial, owner_rows)
    per = n // t // 2

    def reduce_pair(block):
        rows_of(partial, block_rows)(block)[...] = jnp.dot(
            projected_view(block)[...], values[...], preferred_element_type=F32
        )
        for j in range(per):
            target = block * per + j
            out_y_view(target)[...] = partial_view(target * 2 + 1 - parity)[...].astype(BF16)
            copy = remote(
                out_y_view(target), in_y_view(target), y_send.at[target], y_recv.at[target], "fs", partner
            )
            copy.start()
            pending.append(copy)

    def reduce_groups(block):
        for j in range(per):
            target = block * per + j
            remote(
                out_y_view(target), in_y_view(target), y_send.at[target], y_recv.at[target], "fs", partner
            ).wait_recv()
            mine = partial_view(target * 2 + parity)
            mine[...] = mine[...] + in_y_view(target)[...].astype(F32)
            out_z_view(target)[...] = mine[...].astype(BF16)

            @pl.when(target != group)
            def _():
                remote(
                    out_z_view(target),
                    in_z_view(group),
                    z_send.at[target],
                    z_recv.at[group],
                    "fs",
                    target * 2 + parity,
                ).start()

    loads[4].wait()
    reduce_pair(tp)
    waiting = [tp]
    blocks = b.arrivals()
    for number in range(1, t):
        block = next(blocks)
        reduce_pair(block)
        waiting.append(block)
        if number % 2 == 1:
            for each in waiting:
                reduce_groups(each)
            waiting = []
    for _ in blocks:
        pass

    p.finish()
    decay_sum = decay_parts[0].astype(F32)
    for i in range(1, n):
        decay_sum += decay_parts[i].astype(F32)
    decay_grad_ref[:, decay_columns] = decay_sum
    q = Spread("tp", t, columns_of(decay_grad_ref, decay_width), q_send, q_recv, pending)
    q.start()
    for _ in own.arrivals():
        pass

    loads[5].wait()
    loads[6].wait()
    grad = partial_view(fs)[...]
    for step in range(1, n // 2):
        source = (group + step) % (n // 2)
        remote(
            out_z_view(source), in_z_view(source), z_send.at[source], z_recv.at[source], "fs", source * 2 + parity
        ).wait_recv()
        grad += in_z_view(source)[...].astype(F32)
    grad_ref[...] = grad
    mean_new, var_new = moments(mean[...], var[...], grad)
    adam_ratio = mean_new / (jnp.sqrt(var_new) + 1e-08)
    ratio_view = rows_of(ratio, owner_rows)
    ratio_view(fs)[...] = adam_ratio.astype(BF16)
    d = Gather("fs", n, ratio_view, d_send, d_recv, pending)
    d.start()

    squares = adam_ratio * adam_ratio
    squares = sum(squares[i : i + 8] for i in range(0, squares.shape[0], 8))
    square_tp[tp] = sum(squares[:, i : i + 128] for i in range(0, squares.shape[1], 128))
    st = Spread("tp", t, lambda i: square_tp.at[i], st_send, st_recv, pending)
    st.start()
    st.finish()
    square_fs[fs] = sum(square_tp[i] for i in range(t))
    sf = Spread("fs", n, lambda i: square_fs.at[i], sf_send, sf_recv, pending)
    sf.start()

    for _ in d.arrivals():
        pass
    delta_ref[...] = jnp.dot(own_rows[...], ratio[...], preferred_element_type=F32)
    sf.finish()
    square_ref[...] = sum(square_fs[i] for i in range(n))
    q.finish()
    for copy in pending:
        copy.wait_send()
    for step in range(1, n // 2):
        target = (group + step) % (n // 2)
        remote(
            out_z_view(target), in_z_view(target), z_send.at[target], z_recv.at[target], "fs", target * 2 + parity
        ).wait_send()


def finish(entries, *refs):
    ins, outs, held, made, in_sems, out_sems = refs[:10], refs[10:19], refs[19:29], refs[29:38], refs[38], refs[39]
    loads = [pltpu.make_async_copy(a, b, in_sems.at[i]) for i, (a, b) in enumerate(zip(ins, held))]
    stores = [pltpu.make_async_copy(a, b, out_sems.at[i]) for i, (a, b) in enumerate(zip(made, outs))]
    for load in loads:
        load.start()
    delta, square, weight, grad, mean, var, decay_grad, decay_mean, decay_var, decay_weight = held
    step, new, copy, mean_new, var_new, decay_new, decay_copy, decay_mean_new, decay_var_new = made
    for load in loads[:3]:
        load.wait()
    scale = -0.5 / jnp.sqrt(jnp.sum(square[...], keepdims=True) / entries + 1e-06)
    step[...] = scale * delta[...]
    stores[0].start()
    new[...] = weight[...] + step[...]
    stores[1].start()
    copy[...] = new[...].astype(BF16)
    stores[2].start()
    for load in loads[3:]:
        load.wait()
    mean_new[...], var_new[...] = moments(mean[...], var[...], grad[...])
    stores[3].start()
    stores[4].start()
    decay_mean_new[...], decay_var_new[...] = moments(decay_mean[...], decay_var[...], decay_grad[...])
    stores[7].start()
    stores[8].start()
    decay_new[...] = decay_weight[...] - 0.5 * decay_mean_new[...] / (jnp.sqrt(decay_var_new[...]) + 1e-08)
    stores[5].start()
    decay_copy[...] = decay_new[...].astype(BF16)
    stores[6].start()
    for store in stores:
        store.wait()


def finish_by_kernel(entries, *args):
    like = lambda x, dtype=F32: jax.ShapeDtypeStruct(x.shape, dtype)
    weight, mean, decay_weight = args[2], args[4], args[9]
    outs = (
        like(weight),
        like(weight),
        like(weight, BF16),
        like(mean),
        like(mean),
        like(decay_weight),
        like(decay_weight, BF16),
        like(decay_weight),
        like(decay_weight),
    )
    return pl.pallas_call(
        functools.partial(finish, entries),
        out_shape=outs,
        in_specs=[pl.BlockSpec(memory_space=pltpu.HBM)] * 10,
        out_specs=[pl.BlockSpec(memory_space=pltpu.HBM)] * 9,
        scratch_shapes=[pltpu.VMEM(x.shape, x.dtype) for x in args + outs]
        + [pltpu.SemaphoreType.DMA((10,)), pltpu.SemaphoreType.DMA((9,))],
        name="finish",
    )(*args)


def fits(n, t, inputs, decay_cot, factor, mean):
    depth, width = factor.shape
    rank = width * t
    return (
        n % (2 * t) == 0
        and t % 2 == 0
        and mean.shape[0] % 16 == 0
        and mean.shape[1] % 128 == 0
        and mean.shape[0] * n == rank
        and depth % 128 == 0
        and width % 128 == 0
        and inputs.shape[0] % 128 == 0
        and inputs.shape[1] % (128 * t) == 0
        and decay_cot.shape[1] % 16 == 0
    )


def by_kernel(n, t, inputs, values_cot, decay_cot, factor, mean, var):
    tokens, model = inputs.shape
    depth, width = factor.shape
    columns = values_cot.shape[1]
    heads = decay_cot.shape[1]
    rank = width * t
    owner_rows = rank // n
    dma = lambda k: pltpu.SemaphoreType.DMA((k,))
    half = n // 2
    delta, square, grad, decay_grad = pl.pallas_call(
        functools.partial(kernel, n, t),
        out_shape=(
            jax.ShapeDtypeStruct((depth, columns), F32),
            jax.ShapeDtypeStruct((8, 128), F32),
            jax.ShapeDtypeStruct((owner_rows, columns), F32),
            jax.ShapeDtypeStruct((heads, model), F32),
        ),
        in_specs=[pl.BlockSpec(memory_space=pl.ANY)] * 6,
        out_specs=[pl.BlockSpec(memory_space=pltpu.VMEM)] * 4,
        scratch_shapes=[
            pltpu.VMEM((tokens, model), BF16),
            pltpu.VMEM((tokens, columns), BF16),
            pltpu.VMEM((heads, tokens), BF16),
            pltpu.VMEM((owner_rows, columns), F32),
            pltpu.VMEM((owner_rows, columns), F32),
            pltpu.VMEM((model, width), BF16),
            pltpu.VMEM((depth, rank), BF16),
            pltpu.VMEM((tokens, width), F32),
            pltpu.VMEM((rank, tokens), BF16),
            pltpu.VMEM((rank, columns), F32),
            pltpu.VMEM((rank // 2, columns), BF16),
            pltpu.VMEM((rank // 2, columns), BF16),
            pltpu.VMEM((rank // 2, columns), BF16),
            pltpu.VMEM((rank // 2, columns), BF16),
            pltpu.VMEM((rank, columns), BF16),
            pltpu.VMEM((n, heads, model // t), BF16),
            pltpu.VMEM((t, 8, 128), F32),
            pltpu.VMEM((n, 8, 128), F32),
            dma(7),
            dma(n),
            dma(n),
            dma(t),
            dma(t),
            dma(t),
            dma(t),
            dma(half),
            dma(half),
            dma(half),
            dma(half),
            dma(n),
            dma(n),
            dma(n),
            dma(n),
            dma(t),
            dma(t),
            dma(t),
            dma(t),
            dma(n),
            dma(n),
        ],
        compiler_params=pltpu.CompilerParams(collective_id=0, has_side_effects=True),
        name="lowrank",
    )(inputs, values_cot, decay_cot.T, factor, mean, var)
    return delta, square, grad, decay_grad


def by_collectives(inputs, values_cot, decay_cot, factor, mean, var):
    own_rows = lax.all_gather(factor, "tp", axis=1, tiled=True)
    quarter = jnp.dot(
        inputs, lax.all_gather(factor, "fs", axis=0, tiled=True), preferred_element_type=F32
    ).astype(BF16)
    projected = lax.all_gather(quarter, "tp", axis=1, tiled=True)
    grad = lax.psum_scatter(
        lax.dot_general(projected, values_cot, (((0,), (0,)), ((), ())), preferred_element_type=F32),
        "fs",
        scatter_dimension=0,
        tiled=True,
    )
    mean_new, var_new = moments(mean, var, grad)
    adam_ratio = mean_new / (jnp.sqrt(var_new) + 1e-08)
    full_ratio = lax.all_gather(adam_ratio, "fs", axis=0, tiled=True)
    squares = lax.psum(jnp.sum(adam_ratio * adam_ratio), ("fs", "tp"))
    delta = jnp.dot(own_rows.astype(F32), full_ratio, precision=lax.Precision.HIGHEST)
    decay_part = lax.dot_general(inputs, decay_cot, (((0,), (0,)), ((), ())), preferred_element_type=F32)
    return delta, squares, grad, lax.psum(decay_part, "fs")


def local(
    n,
    t,
    inputs,
    values_cot,
    decay_cot,
    factor,
    value_weight,
    lowrank_mean,
    lowrank_var,
    decay_weight,
    decay_mean,
    decay_var,
):
    middle = inputs, values_cot, decay_cot, factor, lowrank_mean, lowrank_var
    entries = lowrank_mean.size * n * t
    if fits(n, t, inputs, decay_cot, factor, lowrank_mean):
        delta, square, lowrank_grad, decay_grad = by_kernel(n, t, *middle)
        outs = finish_by_kernel(
            entries,
            delta,
            square,
            value_weight,
            lowrank_grad,
            lowrank_mean,
            lowrank_var,
            decay_grad,
            decay_mean.T,
            decay_var.T,
            decay_weight.T,
        )
        return outs[:5] + tuple(x.T for x in outs[5:])
    delta, squares, lowrank_grad, decay_grad = by_collectives(*middle)
    mean_new, var_new = moments(lowrank_mean, lowrank_var, lowrank_grad)
    root_mean = jnp.sqrt(squares / entries + 1e-06)
    value_step = -0.5 / root_mean * delta
    value_new = value_weight + value_step
    value_copy = value_new.astype(BF16)
    decay_mean_new, decay_var_new = moments(decay_mean, decay_var, decay_grad)
    decay_new = decay_weight - 0.5 * decay_mean_new / (jnp.sqrt(decay_var_new) + 1e-08)
    decay_copy = decay_new.astype(BF16)
    return (
        value_step,
        value_new,
        value_copy,
        mean_new,
        var_new,
        decay_new,
        decay_copy,
        decay_mean_new,
        decay_var_new,
    )


def solution(mesh):
    in_specs = (
        P("fs", None),
        P("fs", "tp"),
        P("fs", None),
        P("fs", "tp"),
        P("fs", "tp"),
        P("fs", "tp"),
        P("fs", "tp"),
        P(),
        P(),
        P(),
    )
    out_specs = (
        P("fs", "tp"),
        P("fs", "tp"),
        P("fs", "tp"),
        P("fs", "tp"),
        P("fs", "tp"),
        P(),
        P(),
        P(),
        P(),
    )
    body = functools.partial(local, mesh.shape["fs"], mesh.shape["tp"])
    return jax.shard_map(body, mesh=mesh, in_specs=in_specs, out_specs=out_specs, check_vma=False)
```

```python
import functools

import jax
import jax.numpy as jnp
from jax import lax
from jax.experimental import pallas as pl
from jax.experimental.pallas import tpu as pltpu
from jax.sharding import PartitionSpec as P

MESH = pl.DeviceIdType.MESH
F32 = jnp.float32
BF16 = jnp.bfloat16


def moments(mean, var, grad):
    return 0.9 * mean + 0.1 * grad, 0.95 * var + 0.05 * grad * grad


def remote(src, dst, send_sem, recv_sem, axis, peer):
    return pltpu.make_async_remote_copy(
        src_ref=src,
        dst_ref=dst,
        send_sem=send_sem,
        recv_sem=recv_sem,
        device_id={axis: peer},
        device_id_type=MESH,
    )


class Gather:
    def __init__(self, axis, size, view, send_sems, recv_sems, pending):
        self.axis, self.view, self.pending = axis, view, pending
        self.send_sems, self.recv_sems = send_sems, recv_sems
        self.me = lax.axis_index(axis)
        self.groups = size // 2
        self.group, self.parity = self.me // 2, self.me % 2
        self.partner = self.group * 2 + 1 - self.parity
        self.steps = sorted(range(1, self.groups), key=lambda d: min(d, self.groups - d))

    def slot(self, step, parity):
        return (self.group + step) % self.groups * 2 + parity

    def send(self, block, peer, number):
        ref = self.view(block)
        copy = remote(ref, ref, self.send_sems.at[number], self.recv_sems.at[block], self.axis, peer)
        copy.start()
        self.pending.append(copy)

    def wait(self, block):
        ref = self.view(block)
        remote(ref, ref, self.send_sems.at[0], self.recv_sems.at[block], self.axis, self.partner).wait_recv()

    def start(self):
        for number, step in enumerate(self.steps):
            self.send(self.me, self.slot(step, self.parity), number)
        self.send(self.me, self.partner, self.groups - 1)

    def arrivals(self):
        self.wait(self.partner)
        yield self.partner
        for number, step in enumerate(self.steps):
            block = self.slot(step, self.parity)
            self.wait(block)
            self.send(block, self.partner, self.groups + number)
            yield block
        for step in self.steps:
            block = self.slot(step, 1 - self.parity)
            self.wait(block)
            yield block


class Spread:
    def __init__(self, axis, size, view, send_sems, recv_sems, pending):
        self.axis, self.size, self.view, self.pending = axis, size, view, pending
        self.send_sems, self.recv_sems = send_sems, recv_sems
        self.me = lax.axis_index(axis)

    def start(self):
        ref = self.view(self.me)
        for step in range(1, self.size):
            copy = remote(
                ref, ref, self.send_sems.at[step - 1], self.recv_sems.at[self.me], self.axis, (self.me + step) % self.size
            )
            copy.start()
            self.pending.append(copy)

    def finish(self):
        for step in range(1, self.size):
            source = (self.me + step) % self.size
            ref = self.view(source)
            remote(ref, ref, self.send_sems.at[0], self.recv_sems.at[source], self.axis, source).wait_recv()


def rows_of(ref, size):
    return lambda i: ref.at[pl.ds(pl.multiple_of(i * size, size), size)]


def columns_of(ref, size):
    return lambda i: ref.at[:, pl.ds(pl.multiple_of(i * size, size), size)]


def kernel(
    n,
    t,
    inputs_hbm,
    values_hbm,
    decay_hbm,
    factor_hbm,
    mean_hbm,
    var_hbm,
    delta_ref,
    square_ref,
    grad_ref,
    decay_grad_ref,
    inputs,
    values,
    decay,
    mean,
    var,
    quarter,
    own_rows,
    total,
    projected,
    partial,
    out_y,
    in_y,
    out_z,
    in_z,
    ratio,
    decay_parts,
    square_tp,
    square_fs,
    load_sems,
    a_send,
    a_recv,
    o_send,
    o_recv,
    b_send,
    b_recv,
    y_send,
    y_recv,
    z_send,
    z_recv,
    d_send,
    d_recv,
    p_send,
    p_recv,
    q_send,
    q_recv,
    st_send,
    st_recv,
    sf_send,
    sf_recv,
):
    fs, tp = lax.axis_index("fs"), lax.axis_index("tp")
    group, parity = fs // 2, fs % 2
    partner = group * 2 + 1 - parity
    depth, width = factor_hbm.shape
    rank = width * t
    block_rows, owner_rows = rank // t, rank // n
    decay_width = inputs.shape[1] // t
    pending = []

    quarter_view = rows_of(quarter, depth)
    own_view = columns_of(own_rows, width)
    loads = [
        pltpu.make_async_copy(source, target, load_sems.at[i])
        for i, (source, target) in enumerate(
            (
                (factor_hbm, quarter_view(fs)),
                (factor_hbm, own_view(tp)),
                (decay_hbm, decay),
                (inputs_hbm, inputs),
                (values_hbm, values),
                (mean_hbm, mean),
                (var_hbm, var),
            )
        )
    ]
    for load in loads:
        load.start()

    barrier = pltpu.get_barrier_semaphore()
    for step in range(1, t):
        pl.semaphore_signal(barrier, inc=1, device_id={"tp": (tp + step) % t}, device_id_type=MESH)
    for step in range(1, n):
        pl.semaphore_signal(barrier, inc=1, device_id={"fs": (fs + step) % n}, device_id_type=MESH)
    pl.semaphore_wait(barrier, n + t - 2)

    a = Gather("fs", n, quarter_view, a_send, a_recv, pending)
    loads[0].wait()
    a.start()
    own = Gather("tp", t, own_view, o_send, o_recv, pending)
    loads[1].wait()
    own.start()

    loads[2].wait()
    loads[3].wait()
    decay_columns = pl.ds(pl.multiple_of(tp * decay_width, decay_width), decay_width)
    decay_parts[fs] = jnp.dot(decay[...], inputs[:, decay_columns], preferred_element_type=F32).astype(BF16)

    def project(block):
        at = pl.ds(pl.multiple_of(block * depth, depth), depth)
        return jnp.dot(inputs[:, at], quarter[at], preferred_element_type=F32)

    total[...] = project(fs)
    for block in a.arrivals():
        total[...] += project(block)

    projected_view = rows_of(projected, block_rows)
    projected_view(tp)[...] = total[...].T.astype(BF16)
    b = Gather("tp", t, projected_view, b_send, b_recv, pending)
    b.start()
    p = Spread("fs", n, lambda i: decay_parts.at[i], p_send, p_recv, pending)
    p.start()

    out_y_view, in_y_view = rows_of(out_y, owner_rows), rows_of(in_y, owner_rows)
    out_z_view, in_z_view = rows_of(out_z, owner_rows), rows_of(in_z, owner_rows)
    partial_view = rows_of(partial, owner_rows)
    per = n // t // 2

    def reduce_pair(block):
        rows_of(partial, block_rows)(block)[...] = jnp.dot(
            projected_view(block)[...], values[...], preferred_element_type=F32
        )
        for j in range(per):
            target = block * per + j
            out_y_view(target)[...] = partial_view(target * 2 + 1 - parity)[...].astype(BF16)
            copy = remote(
                out_y_view(target), in_y_view(target), y_send.at[target], y_recv.at[target], "fs", partner
            )
            copy.start()
            pending.append(copy)

    def reduce_groups(block):
        for j in range(per):
            target = block * per + j
            remote(
                out_y_view(target), in_y_view(target), y_send.at[target], y_recv.at[target], "fs", partner
            ).wait_recv()
            mine = partial_view(target * 2 + parity)
            mine[...] = mine[...] + in_y_view(target)[...].astype(F32)
            out_z_view(target)[...] = mine[...].astype(BF16)

            @pl.when(target != group)
            def _():
                remote(
                    out_z_view(target),
                    in_z_view(group),
                    z_send.at[target],
                    z_recv.at[group],
                    "fs",
                    target * 2 + parity,
                ).start()

    loads[4].wait()
    reduce_pair(tp)
    before = tp
    blocks = b.arrivals()
    for number in range(1, t):
        block = next(blocks)
        reduce_pair(block)
        reduce_groups(before)
        before = block
    reduce_groups(before)
    for _ in blocks:
        pass

    p.finish()
    decay_sum = decay_parts[0].astype(F32)
    for i in range(1, n):
        decay_sum += decay_parts[i].astype(F32)
    decay_grad_ref[:, decay_columns] = decay_sum
    q = Spread("tp", t, columns_of(decay_grad_ref, decay_width), q_send, q_recv, pending)
    q.start()
    for _ in own.arrivals():
        pass

    loads[5].wait()
    loads[6].wait()
    grad = partial_view(fs)[...]
    for step in range(1, n // 2):
        source = (group + step) % (n // 2)
        remote(
            out_z_view(source), in_z_view(source), z_send.at[source], z_recv.at[source], "fs", source * 2 + parity
        ).wait_recv()
        grad += in_z_view(source)[...].astype(F32)
    grad_ref[...] = grad
    mean_new, var_new = moments(mean[...], var[...], grad)
    adam_ratio = mean_new / (jnp.sqrt(var_new) + 1e-08)
    ratio_view = rows_of(ratio, owner_rows)
    ratio_view(fs)[...] = adam_ratio.astype(BF16)
    d = Gather("fs", n, ratio_view, d_send, d_recv, pending)
    d.start()

    squares = adam_ratio * adam_ratio
    squares = sum(squares[i : i + 8] for i in range(0, squares.shape[0], 8))
    square_tp[tp] = sum(squares[:, i : i + 128] for i in range(0, squares.shape[1], 128))
    st = Spread("tp", t, lambda i: square_tp.at[i], st_send, st_recv, pending)
    st.start()
    st.finish()
    square_fs[fs] = sum(square_tp[i] for i in range(t))
    sf = Spread("fs", n, lambda i: square_fs.at[i], sf_send, sf_recv, pending)
    sf.start()

    for _ in d.arrivals():
        pass
    delta_ref[...] = jnp.dot(own_rows[...], ratio[...], preferred_element_type=F32)
    sf.finish()
    square_ref[...] = sum(square_fs[i] for i in range(n))
    q.finish()
    for copy in pending:
        copy.wait_send()
    for step in range(1, n // 2):
        target = (group + step) % (n // 2)
        remote(
            out_z_view(target), in_z_view(target), z_send.at[target], z_recv.at[target], "fs", target * 2 + parity
        ).wait_send()


def finish(entries, *refs):
    ins, outs, held, made, in_sems, out_sems = refs[:10], refs[10:19], refs[19:29], refs[29:38], refs[38], refs[39]
    loads = [pltpu.make_async_copy(a, b, in_sems.at[i]) for i, (a, b) in enumerate(zip(ins, held))]
    stores = [pltpu.make_async_copy(a, b, out_sems.at[i]) for i, (a, b) in enumerate(zip(made, outs))]
    for load in loads:
        load.start()
    delta, square, weight, grad, mean, var, decay_grad, decay_mean, decay_var, decay_weight = held
    step, new, copy, mean_new, var_new, decay_new, decay_copy, decay_mean_new, decay_var_new = made
    for load in loads[:3]:
        load.wait()
    scale = -0.5 / jnp.sqrt(jnp.sum(square[...], keepdims=True) / entries + 1e-06)
    step[...] = scale * delta[...]
    stores[0].start()
    new[...] = weight[...] + step[...]
    stores[1].start()
    copy[...] = new[...].astype(BF16)
    stores[2].start()
    for load in loads[3:]:
        load.wait()
    mean_new[...], var_new[...] = moments(mean[...], var[...], grad[...])
    stores[3].start()
    stores[4].start()
    decay_mean_new[...], decay_var_new[...] = moments(decay_mean[...], decay_var[...], decay_grad[...])
    stores[7].start()
    stores[8].start()
    decay_new[...] = decay_weight[...] - 0.5 * decay_mean_new[...] / (jnp.sqrt(decay_var_new[...]) + 1e-08)
    stores[5].start()
    decay_copy[...] = decay_new[...].astype(BF16)
    stores[6].start()
    for store in stores:
        store.wait()


def finish_by_kernel(entries, *args):
    like = lambda x, dtype=F32: jax.ShapeDtypeStruct(x.shape, dtype)
    weight, mean, decay_weight = args[2], args[4], args[9]
    outs = (
        like(weight),
        like(weight),
        like(weight, BF16),
        like(mean),
        like(mean),
        like(decay_weight),
        like(decay_weight, BF16),
        like(decay_weight),
        like(decay_weight),
    )
    return pl.pallas_call(
        functools.partial(finish, entries),
        out_shape=outs,
        in_specs=[pl.BlockSpec(memory_space=pltpu.HBM)] * 10,
        out_specs=[pl.BlockSpec(memory_space=pltpu.HBM)] * 9,
        scratch_shapes=[pltpu.VMEM(x.shape, x.dtype) for x in args + outs]
        + [pltpu.SemaphoreType.DMA((10,)), pltpu.SemaphoreType.DMA((9,))],
        name="finish",
    )(*args)


def fits(n, t, inputs, decay_cot, factor, mean):
    depth, width = factor.shape
    rank = width * t
    return (
        n % (2 * t) == 0
        and t % 2 == 0
        and mean.shape[0] % 16 == 0
        and mean.shape[1] % 128 == 0
        and mean.shape[0] * n == rank
        and depth % 128 == 0
        and width % 128 == 0
        and inputs.shape[0] % 128 == 0
        and inputs.shape[1] % (128 * t) == 0
        and decay_cot.shape[1] % 16 == 0
    )


def by_kernel(n, t, inputs, values_cot, decay_cot, factor, mean, var):
    tokens, model = inputs.shape
    depth, width = factor.shape
    columns = values_cot.shape[1]
    heads = decay_cot.shape[1]
    rank = width * t
    owner_rows = rank // n
    dma = lambda k: pltpu.SemaphoreType.DMA((k,))
    half = n // 2
    delta, square, grad, decay_grad = pl.pallas_call(
        functools.partial(kernel, n, t),
        out_shape=(
            jax.ShapeDtypeStruct((depth, columns), F32),
            jax.ShapeDtypeStruct((8, 128), F32),
            jax.ShapeDtypeStruct((owner_rows, columns), F32),
            jax.ShapeDtypeStruct((heads, model), F32),
        ),
        in_specs=[pl.BlockSpec(memory_space=pl.ANY)] * 6,
        out_specs=[pl.BlockSpec(memory_space=pltpu.VMEM)] * 4,
        scratch_shapes=[
            pltpu.VMEM((tokens, model), BF16),
            pltpu.VMEM((tokens, columns), BF16),
            pltpu.VMEM((heads, tokens), BF16),
            pltpu.VMEM((owner_rows, columns), F32),
            pltpu.VMEM((owner_rows, columns), F32),
            pltpu.VMEM((model, width), BF16),
            pltpu.VMEM((depth, rank), BF16),
            pltpu.VMEM((tokens, width), F32),
            pltpu.VMEM((rank, tokens), BF16),
            pltpu.VMEM((rank, columns), F32),
            pltpu.VMEM((rank // 2, columns), BF16),
            pltpu.VMEM((rank // 2, columns), BF16),
            pltpu.VMEM((rank // 2, columns), BF16),
            pltpu.VMEM((rank // 2, columns), BF16),
            pltpu.VMEM((rank, columns), BF16),
            pltpu.VMEM((n, heads, model // t), BF16),
            pltpu.VMEM((t, 8, 128), F32),
            pltpu.VMEM((n, 8, 128), F32),
            dma(7),
            dma(n),
            dma(n),
            dma(t),
            dma(t),
            dma(t),
            dma(t),
            dma(half),
            dma(half),
            dma(half),
            dma(half),
            dma(n),
            dma(n),
            dma(n),
            dma(n),
            dma(t),
            dma(t),
            dma(t),
            dma(t),
            dma(n),
            dma(n),
        ],
        compiler_params=pltpu.CompilerParams(collective_id=0, has_side_effects=True),
        name="lowrank",
    )(inputs, values_cot, decay_cot.T, factor, mean, var)
    return delta, square, grad, decay_grad


def by_collectives(inputs, values_cot, decay_cot, factor, mean, var):
    own_rows = lax.all_gather(factor, "tp", axis=1, tiled=True)
    quarter = jnp.dot(
        inputs, lax.all_gather(factor, "fs", axis=0, tiled=True), preferred_element_type=F32
    ).astype(BF16)
    projected = lax.all_gather(quarter, "tp", axis=1, tiled=True)
    grad = lax.psum_scatter(
        lax.dot_general(projected, values_cot, (((0,), (0,)), ((), ())), preferred_element_type=F32),
        "fs",
        scatter_dimension=0,
        tiled=True,
    )
    mean_new, var_new = moments(mean, var, grad)
    adam_ratio = mean_new / (jnp.sqrt(var_new) + 1e-08)
    full_ratio = lax.all_gather(adam_ratio, "fs", axis=0, tiled=True)
    squares = lax.psum(jnp.sum(adam_ratio * adam_ratio), ("fs", "tp"))
    delta = jnp.dot(own_rows.astype(F32), full_ratio, precision=lax.Precision.HIGHEST)
    decay_part = lax.dot_general(inputs, decay_cot, (((0,), (0,)), ((), ())), preferred_element_type=F32)
    return delta, squares, grad, lax.psum(decay_part, "fs")


def local(
    n,
    t,
    inputs,
    values_cot,
    decay_cot,
    factor,
    value_weight,
    lowrank_mean,
    lowrank_var,
    decay_weight,
    decay_mean,
    decay_var,
):
    middle = inputs, values_cot, decay_cot, factor, lowrank_mean, lowrank_var
    entries = lowrank_mean.size * n * t
    if fits(n, t, inputs, decay_cot, factor, lowrank_mean):
        delta, square, lowrank_grad, decay_grad = by_kernel(n, t, *middle)
        outs = finish_by_kernel(
            entries,
            delta,
            square,
            value_weight,
            lowrank_grad,
            lowrank_mean,
            lowrank_var,
            decay_grad,
            decay_mean.T,
            decay_var.T,
            decay_weight.T,
        )
        return outs[:5] + tuple(x.T for x in outs[5:])
    delta, squares, lowrank_grad, decay_grad = by_collectives(*middle)
    mean_new, var_new = moments(lowrank_mean, lowrank_var, lowrank_grad)
    root_mean = jnp.sqrt(squares / entries + 1e-06)
    value_step = -0.5 / root_mean * delta
    value_new = value_weight + value_step
    value_copy = value_new.astype(BF16)
    decay_mean_new, decay_var_new = moments(decay_mean, decay_var, decay_grad)
    decay_new = decay_weight - 0.5 * decay_mean_new / (jnp.sqrt(decay_var_new) + 1e-08)
    decay_copy = decay_new.astype(BF16)
    return (
        value_step,
        value_new,
        value_copy,
        mean_new,
        var_new,
        decay_new,
        decay_copy,
        decay_mean_new,
        decay_var_new,
    )


def solution(mesh):
    in_specs = (
        P("fs", None),
        P("fs", "tp"),
        P("fs", None),
        P("fs", "tp"),
        P("fs", "tp"),
        P("fs", "tp"),
        P("fs", "tp"),
        P(),
        P(),
        P(),
    )
    out_specs = (
        P("fs", "tp"),
        P("fs", "tp"),
        P("fs", "tp"),
        P("fs", "tp"),
        P("fs", "tp"),
        P(),
        P(),
        P(),
        P(),
    )
    body = functools.partial(local, mesh.shape["fs"], mesh.shape["tp"])
    return jax.shard_map(body, mesh=mesh, in_specs=in_specs, out_specs=out_specs, check_vma=False)
```
